32 devices in a mesh: sp: 8 (over z, x), tp: 4 (over y, core).
Axes of the slice: x: 2, y: 2, z: 4, core: 2. Of those that a mesh axis runs over, the one named last changes fastest.
Arguments:
- queries: bfloat16 [2048, 1024], P('sp', 'tp'), may hold values from -9 to 9
- keys: bfloat16 [2048, 512], P('sp', 'tp'), may hold values from -9 to 9
- values: bfloat16 [2048, 512], P('sp', 'tp'), may hold values from -6 to 6
- residual: bfloat16 [2048, 2048], P(('sp', 'tp')), may hold values from -6 to 6
- query_gain: float32 [128], replicated, may hold values from 1 to 5
- key_gain: float32 [128], replicated, may hold values from 1 to 5
- out_weight: bfloat16 [1024, 2048], replicated, may hold values from -0.1875 to 0.1875
- first_gain: float32 [2048], replicated, may hold values from 0.1 to 1.9
- first_bias: float32 [2048], replicated, may hold values from -3 to 3
- up_weight: bfloat16 [2048, 8192], P('sp', 'tp'), may hold values from -0.125 to 0.125
- down_weight: bfloat16 [2048, 8192], P('sp', 'tp'), may hold values from -0.0625 to 0.0625
- second_gain: float32 [2048], replicated, may hold values from 0.1 to 1.9
- second_bias: float32 [2048], replicated, may hold values from -3 to 3
Outputs:
- layer_out: bfloat16 [2048, 2048], P(('sp', 'tp'))
The draws below stay inside these ranges and needn't reach their ends.
All inputs are finite; a program needn't handle non-finite values.
Results may differ from the reference program's by a relative error of at most 0.015.
Values may be sent and summed in bfloat16 or wider, within the bound.
A program may use at most 128 MiB of HBM per device.

```python
import math
import jax
import jax.numpy as jnp
from jax import lax

D = 2048
HEADS = 8
KV_HEADS = 4
HEAD_DIM = 128
FF = 8192
GRID_W = 64
TOKENS = 2048


def draw_queries(key, part):
    noise = jnp.clip(jax.random.normal(jax.random.fold_in(key, 1), (TOKENS, HEADS * HEAD_DIM), jnp.float32), -6.0, 6.0)
    return noise.astype(jnp.bfloat16)


def draw_keys(key, part):
    noise = jnp.clip(jax.random.normal(jax.random.fold_in(key, 2), (TOKENS, KV_HEADS * HEAD_DIM), jnp.float32), -6.0, 6.0)
    return noise.astype(jnp.bfloat16)


def level_of(stream_key, shape, shards, smallest, top_value):
    level, own = 1.0, jax.random.fold_in(stream_key, 6)
    for axis_at, blocks in shards:
        heights = jnp.exp(jax.random.uniform(jax.random.fold_in(own, axis_at), (blocks,), jnp.float32, smallest / len(shards), top_value / len(shards)))
        level = level * jnp.repeat(heights, shape[axis_at] // blocks).reshape([-1 if axis == axis_at else 1 for axis in range(len(shape))])
    return level


def bell_draw(key, extent, width, limit, cuts=(), held_as=jnp.bfloat16):
    values = jax.random.normal(key, extent, jnp.float32) * width
    if len(cuts) > 0:
        values = level_of(key, extent, cuts, -0.22, 0.18) * values
    return jnp.clip(values, min=-limit, max=limit).astype(held_as)


def setup_inputs(seed: int = 0) -> dict:
    streams_of = jax.random.split(jax.random.key(seed), 14)
    queries = draw_queries(jax.random.fold_in(streams_of[13], 71), 0)
    keys = draw_keys(jax.random.fold_in(streams_of[13], 71), 0)
    values = bell_draw(streams_of[2], (TOKENS, KV_HEADS * HEAD_DIM), 1.0, 6.0, ((0, 8), (1, 4)))
    residual = bell_draw(streams_of[3], (TOKENS, D), 1.0, 6.0, ((0, 32),))
    query_gain = jnp.clip(jax.random.uniform(streams_of[4], (HEAD_DIM,), jnp.float32, 1.0, 5.0), 1.0, 5.0)
    key_gain = jnp.clip(jax.random.uniform(streams_of[5], (HEAD_DIM,), jnp.float32, 1.0, 5.0), 1.0, 5.0)
    out_weight = bell_draw(streams_of[6], (HEADS * HEAD_DIM, D), (HEADS * HEAD_DIM) ** -0.5, 0.1875)
    first_gain = jnp.clip(1.0 + 0.18 * jax.random.normal(streams_of[7], (D,), jnp.float32), 0.1, 1.9)
    first_bias = bell_draw(streams_of[8], (D,), 0.5, 3.0, (), jnp.float32)
    up_weight = bell_draw(streams_of[9], (D, FF), D ** -0.5, 0.125, ((0, 8), (1, 4)))
    down_weight = bell_draw(streams_of[10], (D, FF), FF ** -0.5, 0.0625, ((0, 8), (1, 4)))
    second_gain = jnp.clip(1.0 + 0.18 * jax.random.normal(streams_of[11], (D,), jnp.float32), 0.1, 1.9)
    second_bias = bell_draw(streams_of[12], (D,), 0.5, 3.0, (), jnp.float32)
    return dict(queries=queries, keys=keys, values=values, residual=residual, query_gain=query_gain, key_gain=key_gain, out_weight=out_weight, first_gain=first_gain, first_bias=first_bias, up_weight=up_weight, down_weight=down_weight, second_gain=second_gain, second_bias=second_bias)


RESIDUAL_SCALE = 2.0 ** 0.25
LAYER_EPS = 1e-05
HEAD_EPS = 1e-06
ROTARY_BASE = 10000.0

def grid_angles(positions, head_dim):
    quarter = head_dim // 4
    inverse = ROTARY_BASE ** (-jnp.arange(quarter, dtype=jnp.float32) / quarter)
    grid_row = (positions // GRID_W).astype(jnp.float32)
    grid_col = (positions % GRID_W).astype(jnp.float32)
    return jnp.concatenate([grid_row[:, None] * inverse, grid_col[:, None] * inverse], axis=-1)

def norm_rotate(projected, gain, angles, head_dim):
    row_count = projected.shape[0]
    head_count = projected.shape[1] // head_dim
    as_float = projected.astype(jnp.float32).reshape(row_count, head_count, head_dim)
    normed = as_float * lax.rsqrt(lax.optimization_barrier(jnp.mean(as_float * as_float, axis=-1, keepdims=True)) + HEAD_EPS) * gain
    paired = normed.reshape(row_count, head_count, head_dim // 2, 2)
    cosine = jnp.cos(angles)[:, None, :]
    sine = jnp.sin(angles)[:, None, :]
    even_part = paired[..., 0]
    odd_part = paired[..., 1]
    turned = jnp.stack([even_part * cosine - odd_part * sine, even_part * sine + odd_part * cosine], axis=-1)
    return turned.reshape(row_count, head_count, head_dim).astype(jnp.bfloat16)

def layer_norm(summed, gain, bias):
    centred = summed - lax.optimization_barrier(jnp.mean(summed, axis=-1, keepdims=True))
    variance = lax.optimization_barrier(jnp.mean(centred * centred, axis=-1, keepdims=True))
    return centred * lax.rsqrt(variance + LAYER_EPS) * gain + bias

def reference(queries, keys, values, residual, query_gain, key_gain, out_weight, first_gain, first_bias, up_weight, down_weight, second_gain, second_bias):
    positions = jnp.arange(TOKENS, dtype=jnp.int32)
    angles = grid_angles(positions, HEAD_DIM)
    query_rot = norm_rotate(queries, query_gain, angles, HEAD_DIM)
    key_float = norm_rotate(keys, key_gain, angles, HEAD_DIM).astype(jnp.float32)
    value_rows = values.reshape(TOKENS, KV_HEADS, HEAD_DIM).astype(jnp.float32)
    group = HEADS // KV_HEADS
    block_rows = math.gcd(TOKENS, 256)
    score_scale = HEAD_DIM ** (-0.5)

    def one_block(begin):
        query_block = lax.dynamic_slice_in_dim(query_rot, begin, block_rows, 0).astype(jnp.float32)
        query_block = query_block.reshape(block_rows, KV_HEADS, group, HEAD_DIM)
        scores = jnp.einsum('qkgd,skd->kgqs', query_block, key_float) * score_scale
        largest = lax.optimization_barrier(jnp.max(scores, axis=-1, keepdims=True))
        weights = jnp.exp(scores - largest)
        total = lax.optimization_barrier(jnp.sum(weights, axis=-1))
        rounded = lax.optimization_barrier(weights.astype(jnp.bfloat16)).astype(jnp.float32)
        summed = jnp.einsum('kgqs,skd->kgqd', rounded, value_rows)
        result = summed / total[..., None]
        return jnp.transpose(result, (2, 0, 1, 3)).reshape(block_rows, HEADS * HEAD_DIM).astype(jnp.bfloat16)
    starts = jnp.arange(TOKENS // block_rows, dtype=jnp.int32) * block_rows
    attended = lax.map(one_block, starts).reshape(TOKENS, HEADS * HEAD_DIM)
    mixed = jnp.dot(attended, out_weight, preferred_element_type=jnp.float32)
    first_norm = layer_norm(RESIDUAL_SCALE * residual.astype(jnp.float32) + mixed, first_gain, first_bias).astype(jnp.bfloat16)
    up_values = jnp.dot(first_norm, up_weight, preferred_element_type=jnp.float32)
    hidden = jnp.square(jnp.maximum(up_values, 0.0)).astype(jnp.bfloat16)
    channel_out = lax.dot_general(hidden, down_weight, (((1,), (1,)), ((), ())), preferred_element_type=jnp.float32)
    layer_out = layer_norm(RESIDUAL_SCALE * first_norm.astype(jnp.float32) + channel_out, second_gain, second_bias)
    return layer_out.astype(jnp.bfloat16)
```

```python
import functools
import math

import jax
import jax.numpy as jnp
from jax import lax
from jax.experimental import pallas as pl
from jax.experimental.pallas import tpu as pltpu
from jax.sharding import PartitionSpec as P

HEAD_DIM = 128
GRID_W = 64
RESIDUAL_SCALE = 2.0**0.25
LAYER_EPS = 1e-05
HEAD_EPS = 1e-06
ROTARY_BASE = 10000.0
MESH = pl.DeviceIdType.MESH


def grid_tables(positions):
    quarter = HEAD_DIM // 4
    lane = jnp.arange(HEAD_DIM, dtype=jnp.int32)
    pair = lane // 2
    inverse = ROTARY_BASE ** (-(pair % quarter).astype(jnp.float32) / quarter)
    grid_row = (positions // GRID_W).astype(jnp.float32)
    grid_col = (positions % GRID_W).astype(jnp.float32)
    angles = jnp.where(pair < quarter, grid_row[:, None], grid_col[:, None]) * inverse
    sign = jnp.where(lane % 2 == 0, -1.0, 1.0)
    return jnp.cos(angles), jnp.sin(angles) * sign


def turn(block, gain, cosine, sine):
    x = block.astype(jnp.float32)
    x = x * lax.rsqrt(jnp.mean(x * x, axis=-1, keepdims=True) + HEAD_EPS) * gain
    lane = lax.broadcasted_iota(jnp.int32, x.shape, 1)
    swapped = jnp.where(
        lane % 2 == 0, pltpu.roll(x, HEAD_DIM - 1, 1), pltpu.roll(x, 1, 1)
    )
    return (x * cosine + swapped * sine).astype(jnp.bfloat16)


def layer_norm(summed, gain, bias):
    centred = summed - jnp.mean(summed, axis=-1, keepdims=True)
    variance = jnp.mean(centred * centred, axis=-1, keepdims=True)
    return centred * lax.rsqrt(variance + LAYER_EPS) * gain + bias


def kernel(
    dims,
    q_ref, k_ref, v_ref, res_ref, cos_ref, sin_ref, qg_ref, kg_ref, wo_hbm,
    g1_ref, b1_ref, up_hbm, down_hbm, g2_ref, b2_ref,
    out_ref,
    kv, wup, wdn, wo, att, att_in, mixed, rows, part, rl, s1, rh, s2, rz,
    local_sem, kvz_s, kvz_r, kvx_s, kvx_r, wz_s, wz_r, wx_s, wx_r,
    at_s, at_r, gz_s, gz_r, gh_s, gh_r, gl_s, gl_r,
    rl_s, rl_r, rh_s, rh_r, rz_s, rz_r,
):
    A, B, H = dims
    L = 2
    NT = H * L
    R = q_ref.shape[0]
    CH = q_ref.shape[1]
    Q = R // NT
    D = wup.shape[0]
    DB = up_hbm.shape[0]
    W = wup.shape[1]
    sp = lax.axis_index("sp")
    tp = lax.axis_index("tp")
    a, b = lax.div(sp, B), lax.rem(sp, B)
    h, l = lax.div(tp, L), lax.rem(tp, L)
    sends = []

    def a_to(d):
        return lax.rem(a + d, A)

    def a_from(d):
        return lax.rem(a + A - d, A)

    def remote(src, dst, ssem, rsem, a_, b_, t_):
        copy = pltpu.make_async_remote_copy(
            src_ref=src, dst_ref=dst, send_sem=ssem, recv_sem=rsem,
            device_id={"sp": a_ * B + b_, "tp": t_}, device_id_type=MESH,
        )
        copy.start()
        sends.append(copy)
        return copy

    def ff_cols(a_):
        return pl.ds(pl.multiple_of(a_ * W, 128), W)

    def d_rows(a_, b_):
        return pl.ds(pl.multiple_of((a_ * B + b_) * DB, DB), DB)

    def kv_rows(a_, b_):
        return pl.ds(pl.multiple_of((a_ * B + b_) * R, R), R)

    def tok_rows(a_, h_, l_):
        return pl.ds(pl.multiple_of(((a_ * H + h_) * L + l_) * Q, Q), Q)

    weights = ((up_hbm, wup), (down_hbm, wdn))
    locals_ = [pltpu.make_async_copy(wo_hbm, wo, local_sem.at[0])]
    for i, (src, dst) in enumerate(weights):
        locals_.append(
            pltpu.make_async_copy(
                src.at[:, ff_cols(a)], dst.at[d_rows(a, b), :], local_sem.at[1 + i]
            )
        )
    for copy in locals_:
        copy.start()

    barrier = pltpu.get_barrier_semaphore()
    peers = [(a_to(d), b, tp) for d in range(1, A)]
    peers += [(a, lax.rem(b + e, B), tp) for e in range(1, B)]
    peers += [(a, b, lax.rem(tp + e, NT)) for e in range(1, NT)]
    for a_, b_, t_ in peers:
        pl.semaphore_signal(
            barrier, inc=1, device_id={"sp": a_ * B + b_, "tp": t_}, device_id_type=MESH
        )

    mine = kv_rows(a, b)
    kv[0, mine, :] = turn(k_ref[...], kg_ref[...], cos_ref[...], sin_ref[...])
    kv[1, mine, :] = v_ref[...]
    pl.semaphore_wait(barrier, len(peers))

    kvz = {}
    for d in range(1, A):
        ref = kv.at[:, kv_rows(a, b), :]
        kvz[d] = remote(ref, ref, kvz_s.at[d], kvz_r.at[d], a_to(d), b, tp)

    def kv_forward(d):
        ref = kv.at[:, kv_rows(a_from(d), b), :]
        return [
            remote(ref, ref, kvx_s.at[d, e], kvx_r.at[d, e], a, lax.rem(b + e, B), tp)
            for e in range(1, B)
        ]

    kvx = {0: kv_forward(0)}
    wz, wx = {}, {}
    for i, (src, dst) in enumerate(weights):
        for d in range(1, A):
            wz[i, d] = remote(
                src.at[:, ff_cols(a_to(d))], dst.at[d_rows(a, b), :],
                wz_s.at[i, d], wz_r.at[i, d], a_to(d), b, tp,
            )
        wx[i, 0] = [
            remote(
                src.at[:, ff_cols(a)], dst.at[d_rows(a, b), :],
                wx_s.at[i, 0, e], wx_r.at[i, 0, e], a, lax.rem(b + e, B), tp,
            )
            for e in range(1, B)
        ]

    def w_forward(i, d):
        wz[i, d].wait_recv()
        ref = weights[i][1].at[d_rows(a_from(d), b), :]
        wx[i, d] = [
            remote(ref, ref, wx_s.at[i, d, e], wx_r.at[i, d, e], a, lax.rem(b + e, B), tp)
            for e in range(1, B)
        ]

    heads = CH // HEAD_DIM
    query = jnp.concatenate(
        [
            turn(
                q_ref[:, i * HEAD_DIM : (i + 1) * HEAD_DIM],
                qg_ref[...], cos_ref[...], sin_ref[...],
            )
            for i in range(heads)
        ],
        axis=0,
    )
    factor2 = HEAD_DIM**-0.5 * math.log2(math.e)
    keys_at_once = min(B, 2) * R
    state = (
        jnp.full((heads * R, 1), -1e30, jnp.float32),
        jnp.zeros((heads * R, 1), jnp.float32),
        jnp.zeros((heads * R, HEAD_DIM), jnp.float32),
    )
    for d in range(A):
        for copy in kvx[d]:
            copy.wait_recv()
        if d + 1 < A:
            kvz[d + 1].wait_recv()
            kvx[d + 1] = kv_forward(d + 1)

        def attend(step, carried, d=d):
            running, total, summed = carried
            at = pl.ds(
                pl.multiple_of(a_from(d) * (B * R) + step * keys_at_once, R), keys_at_once
            )
            scores = lax.dot_general(
                query, kv[0, at, :], (((1,), (1,)), ((), ())),
                preferred_element_type=jnp.float32,
            )
            newest = jnp.maximum(running, jnp.max(scores, axis=-1, keepdims=True))
            scale = jnp.exp2((running - newest) * factor2)
            exps = jnp.exp2((scores - newest) * factor2)
            total = total * scale + jnp.sum(exps, axis=-1, keepdims=True)
            summed = summed * scale + jnp.dot(
                exps.astype(jnp.bfloat16), kv[1, at, :], preferred_element_type=jnp.float32
            )
            return newest, total, summed

        steps = (B * R) // keys_at_once
        if steps == 1:
            state = attend(0, state)
        else:
            state = lax.fori_loop(0, steps, attend, state)
    attended = (state[2] / state[1]).astype(jnp.bfloat16)
    for i in range(heads):
        for t in range(NT):
            begin = i * R + t * Q
            att[t, :, i * HEAD_DIM : (i + 1) * HEAD_DIM] = attended[begin : begin + Q, :]

    here = pl.ds(pl.multiple_of(tp * CH, 128), CH)
    att_copies = []
    for e in range(1, NT):
        t_ = lax.rem(tp + e, NT)
        att_copies.append(
            remote(att.at[t_], att_in.at[:, here], at_s.at[e], at_r.at[e], a, b, t_)
        )
    att_in[:, here] = att[tp]
    locals_[0].wait()
    for copy in att_copies:
        copy.wait_recv()

    tile = 512

    def out_tile(n, carried):
        cols = pl.ds(pl.multiple_of(n * tile, tile), tile)
        mixed[:, cols] = jnp.dot(
            att_in[...], wo[:, cols], preferred_element_type=jnp.float32
        )
        return carried

    lax.fori_loop(0, D // tile, out_tile, 0)
    first = layer_norm(
        RESIDUAL_SCALE * res_ref[...].astype(jnp.float32) + mixed[...], g1_ref[...], b1_ref[...]
    ).astype(jnp.bfloat16)
    own_rows = tok_rows(a, h, l)
    rows[own_rows, :] = first

    gz, gh, gl = {}, {}, {}
    for d in range(1, A):
        ref = rows.at[own_rows, :]
        gz[d] = remote(ref, ref, gz_s.at[d], gz_r.at[d], a_to(d), b, tp)

    def gl_forward(d, e):
        ref = rows.at[tok_rows(a_from(d), lax.rem(h + H - e, H), l), :]
        gl[d, e] = remote(ref, ref, gl_s.at[d, e], gl_r.at[d, e], a, b, h * L + (1 - l))

    def gh_forward(d):
        ref = rows.at[tok_rows(a_from(d), h, l), :]
        for e in range(1, H):
            gh[d, e] = remote(
                ref, ref, gh_s.at[d, e], gh_r.at[d, e], a, b, lax.rem(h + e, H) * L + l
            )
        gl_forward(d, 0)

    gh_forward(0)
    for i in range(2):
        for d in range(1, A):
            w_forward(i, d)
    for d in range(1, A):
        gz[d].wait_recv()
        gh_forward(d)
        for e in range(1, H):
            gh[d - 1, e].wait_recv()
            gl_forward(d - 1, e)
    for e in range(1, H):
        gh[A - 1, e].wait_recv()
        gl_forward(A - 1, e)
    for copy in locals_[1:]:
        copy.wait()
    for i in range(2):
        for d in range(A):
            for copy in wx[i, d]:
                copy.wait_recv()

    block = NT * Q
    lsend, hsend, zsend = {}, {}, {}
    order = list(range(1, A)) + [0]

    def mixer(d):
        g = (A - d) % A
        for e in range(H):
            gl[g, e].wait_recv()
        at = a_to(d)
        up = jnp.dot(
            rows[pl.ds(pl.multiple_of(at * block, block), block), :], wup[...],
            preferred_element_type=jnp.float32,
        )
        hidden = jnp.square(jnp.maximum(up, 0.0)).astype(jnp.bfloat16)

        def down_tile(n, carried):
            cols = pl.ds(pl.multiple_of(n * tile, tile), tile)
            piece = lax.dot_general(
                hidden, wdn[cols, :], (((1,), (1,)), ((), ())),
                preferred_element_type=jnp.float32,
            ).astype(jnp.bfloat16)
            for h_ in range(H):
                for l_ in range(L):
                    begin = (h_ * L + l_) * Q
                    part[d, l_, h_, :, cols] = piece[begin : begin + Q, :]
            return carried

        lax.fori_loop(0, D // tile, down_tile, 0)
        lsend[d] = remote(
            part.at[d, 1 - l], rl.at[d], rl_s.at[d], rl_r.at[d], a, b, h * L + (1 - l)
        )

    def core_sum(d):
        lsend[d].wait_recv()
        for h_ in range(H):
            s1[d, h_] = (
                part[d, l, h_].astype(jnp.float32) + rl[d, h_].astype(jnp.float32)
            ).astype(jnp.bfloat16)
        for e in range(1, H):
            h_ = lax.rem(h + e, H)
            hsend[d, e] = remote(
                s1.at[d, h_], rh.at[d, e], rh_s.at[d, e], rh_r.at[d, e], a, b, h_ * L + l
            )

    def tp_sum(d):
        total = s1[d, h].astype(jnp.float32)
        for e in range(1, H):
            hsend[d, e].wait_recv()
            total = total + rh[d, e].astype(jnp.float32)
        if d == 0:
            return total
        s2[d] = total.astype(jnp.bfloat16)
        zsend[d] = remote(s2.at[d], rz.at[d], rz_s.at[d], rz_r.at[d], a_to(d), b, tp)
        return None

    for i, d in enumerate(order):
        mixer(d)
        if i >= 1:
            core_sum(order[i - 1])
    core_sum(order[-1])
    for d in order[:-1]:
        tp_sum(d)
    total = tp_sum(0)
    for d in range(1, A):
        zsend[d].wait_recv()
        total = total + rz[d].astype(jnp.float32)
    out_ref[...] = layer_norm(
        RESIDUAL_SCALE * rows[own_rows, :].astype(jnp.float32) + total,
        g2_ref[...], b2_ref[...],
    ).astype(jnp.bfloat16)
    for copy in sends:
        copy.wait_send()


def per_device(
    sp_size, tp_size,
    queries, keys, values, residual, query_gain, key_gain, out_weight,
    first_gain, first_bias, up_weight, down_weight, second_gain, second_bias,
):
    A = math.gcd(sp_size, 4)
    B = sp_size // A
    L = 2
    H = tp_size // L
    R, CH = queries.shape
    Q, D = residual.shape
    DB, FFL = up_weight.shape
    W = FFL // A
    T = R * sp_size
    block = tp_size * Q
    positions = lax.axis_index("sp") * R + jnp.arange(R, dtype=jnp.int32)
    cosine, sine = grid_tables(positions)
    dma = pltpu.SemaphoreType.DMA
    bf, f32 = jnp.bfloat16, jnp.float32
    vmem = pl.BlockSpec(memory_space=pltpu.VMEM)
    hbm = pl.BlockSpec(memory_space=pl.ANY)
    scratch = [
        pltpu.VMEM((2, T, HEAD_DIM), bf),
        pltpu.VMEM((D, W), bf),
        pltpu.VMEM((D, W), bf),
        pltpu.VMEM(out_weight.shape, bf),
        pltpu.VMEM((tp_size, Q, CH), bf),
        pltpu.VMEM((Q, tp_size * CH), bf),
        pltpu.VMEM((Q, D), f32),
        pltpu.VMEM((A * block, D), bf),
        pltpu.VMEM((A, L, H, Q, D), bf),
        pltpu.VMEM((A, H, Q, D), bf),
        pltpu.VMEM((A, H, Q, D), bf),
        pltpu.VMEM((A, H, Q, D), bf),
        pltpu.VMEM((A, Q, D), bf),
        pltpu.VMEM((A, Q, D), bf),
        dma((3,)),
        dma((A,)), dma((A,)), dma((A, B)), dma((A, B)),
        dma((2, A)), dma((2, A)), dma((2, A, B)), dma((2, A, B)),
        dma((tp_size,)), dma((tp_size,)),
        dma((A,)), dma((A,)), dma((A, H)), dma((A, H)), dma((A, H)), dma((A, H)),
        dma((A,)), dma((A,)), dma((A, H)), dma((A, H)), dma((A,)), dma((A,)),
    ]
    as_row = lambda x: x.reshape(1, -1)
    return pl.pallas_call(
        functools.partial(kernel, (A, B, H)),
        out_shape=jax.ShapeDtypeStruct((Q, D), bf),
        in_specs=[vmem] * 8 + [hbm] + [vmem] * 2 + [hbm] * 2 + [vmem] * 2,
        out_specs=vmem,
        scratch_shapes=scratch,
        compiler_params=pltpu.CompilerParams(
            collective_id=0, has_side_effects=True, vmem_limit_bytes=60000 * 1024
        ),
        name="layer",
    )(
        queries, keys, values, residual, cosine, sine, as_row(query_gain), as_row(key_gain),
        out_weight, as_row(first_gain), as_row(first_bias), up_weight, down_weight,
        as_row(second_gain), as_row(second_bias),
    )


def solution(mesh):
    both = P("sp", "tp")
    split_rows = P(("sp", "tp"), None)
    in_specs = (
        both, both, both, split_rows, P(), P(), P(), P(), P(), both, both, P(), P(),
    )
    return jax.shard_map(
        functools.partial(per_device, mesh.shape["sp"], mesh.shape["tp"]),
        mesh=mesh, in_specs=in_specs, out_specs=split_rows, check_vma=False,
    )
```

```python
import functools
import math

import jax
import jax.numpy as jnp
from jax import lax
from jax.experimental import pallas as pl
from jax.experimental.pallas import tpu as pltpu
from jax.sharding import PartitionSpec as P

HEAD_DIM = 128
GRID_W = 64
RESIDUAL_SCALE = 2.0**0.25
LAYER_EPS = 1e-05
HEAD_EPS = 1e-06
ROTARY_BASE = 10000.0
MESH = pl.DeviceIdType.MESH


def grid_tables(positions):
    quarter = HEAD_DIM // 4
    lane = jnp.arange(HEAD_DIM, dtype=jnp.int32)
    pair = lane // 2
    inverse = ROTARY_BASE ** (-(pair % quarter).astype(jnp.float32) / quarter)
    grid_row = (positions // GRID_W).astype(jnp.float32)
    grid_col = (positions % GRID_W).astype(jnp.float32)
    angles = jnp.where(pair < quarter, grid_row[:, None], grid_col[:, None]) * inverse
    sign = jnp.where(lane % 2 == 0, -1.0, 1.0)
    return jnp.cos(angles), jnp.sin(angles) * sign


def turn(block, gain, cosine, sine):
    x = block.astype(jnp.float32)
    x = x * lax.rsqrt(jnp.mean(x * x, axis=-1, keepdims=True) + HEAD_EPS) * gain
    lane = lax.broadcasted_iota(jnp.int32, x.shape, 1)
    swapped = jnp.where(
        lane % 2 == 0, pltpu.roll(x, HEAD_DIM - 1, 1), pltpu.roll(x, 1, 1)
    )
    return (x * cosine + swapped * sine).astype(jnp.bfloat16)


def layer_norm(summed, gain, bias):
    centred = summed - jnp.mean(summed, axis=-1, keepdims=True)
    variance = jnp.mean(centred * centred, axis=-1, keepdims=True)
    return centred * lax.rsqrt(variance + LAYER_EPS) * gain + bias


def kernel(
    dims,
    q_ref, k_ref, v_ref, res_ref, cos_ref, sin_ref, qg_ref, kg_ref, wo_hbm,
    g1_ref, b1_ref, up_hbm, down_hbm, g2_ref, b2_ref,
    out_ref,
    kv, wup, wdn, wo, att, att_in, mixed, rows, hid, part, rl, s1, rh, s2, rz,
    local_sem, kvz_s, kvz_r, kvx_s, kvx_r, wz_s, wz_r, wx_s, wx_r,
    at_s, at_r, gz_s, gz_r, gh_s, gh_r, gl_s, gl_r,
    rl_s, rl_r, rh_s, rh_r, rz_s, rz_r,
):
    A, B, H = dims
    L = 2
    NT = H * L
    R = q_ref.shape[0]
    CH = q_ref.shape[1]
    Q = R // NT
    D = wup.shape[0]
    DB = up_hbm.shape[0]
    W = wup.shape[1]
    sp = lax.axis_index("sp")
    tp = lax.axis_index("tp")
    a, b = lax.div(sp, B), lax.rem(sp, B)
    h, l = lax.div(tp, L), lax.rem(tp, L)
    sends = []

    def a_to(d):
        return lax.rem(a + d, A)

    def a_from(d):
        return lax.rem(a + A - d, A)

    def remote(src, dst, ssem, rsem, a_, b_, t_):
        copy = pltpu.make_async_remote_copy(
            src_ref=src, dst_ref=dst, send_sem=ssem, recv_sem=rsem,
            device_id={"sp": a_ * B + b_, "tp": t_}, device_id_type=MESH,
        )
        copy.start()
        sends.append(copy)
        return copy

    def ff_cols(a_):
        return pl.ds(pl.multiple_of(a_ * W, 128), W)

    def d_rows(a_, b_):
        return pl.ds(pl.multiple_of((a_ * B + b_) * DB, DB), DB)

    def kv_rows(a_, b_):
        return pl.ds(pl.multiple_of((a_ * B + b_) * R, R), R)

    def tok_rows(a_, h_, l_):
        return pl.ds(pl.multiple_of(((a_ * H + h_) * L + l_) * Q, Q), Q)

    weights = ((up_hbm, wup), (down_hbm, wdn))
    locals_ = [pltpu.make_async_copy(wo_hbm, wo, local_sem.at[0])]
    for i, (src, dst) in enumerate(weights):
        locals_.append(
            pltpu.make_async_copy(
                src.at[:, ff_cols(a)], dst.at[d_rows(a, b), :], local_sem.at[1 + i]
            )
        )
    for copy in locals_:
        copy.start()

    barrier = pltpu.get_barrier_semaphore()
    peers = [(a_to(d), b, tp) for d in range(1, A)]
    peers += [(a, lax.rem(b + e, B), tp) for e in range(1, B)]
    peers += [(a, b, lax.rem(tp + e, NT)) for e in range(1, NT)]
    for a_, b_, t_ in peers:
        pl.semaphore_signal(
            barrier, inc=1, device_id={"sp": a_ * B + b_, "tp": t_}, device_id_type=MESH
        )

    mine = kv_rows(a, b)
    kv[0, mine, :] = turn(k_ref[...], kg_ref[...], cos_ref[...], sin_ref[...])
    kv[1, mine, :] = v_ref[...]
    pl.semaphore_wait(barrier, len(peers))

    kvz = {}
    for d in range(1, A):
        ref = kv.at[:, kv_rows(a, b), :]
        kvz[d] = remote(ref, ref, kvz_s.at[d], kvz_r.at[d], a_to(d), b, tp)

    def kv_forward(d):
        ref = kv.at[:, kv_rows(a_from(d), b), :]
        return [
            remote(ref, ref, kvx_s.at[d, e], kvx_r.at[d, e], a, lax.rem(b + e, B), tp)
            for e in range(1, B)
        ]

    kvx = {0: kv_forward(0)}
    wz, wx = {}, {}
    def w_send(i):
        src, dst = weights[i]
        for d in range(1, A):
            wz[i, d] = remote(
                src.at[:, ff_cols(a_to(d))], dst.at[d_rows(a, b), :],
                wz_s.at[i, d], wz_r.at[i, d], a_to(d), b, tp,
            )

    w_send(0)
    for i, (src, dst) in enumerate(weights):
        wx[i, 0] = [
            remote(
                src.at[:, ff_cols(a)], dst.at[d_rows(a, b), :],
                wx_s.at[i, 0, e], wx_r.at[i, 0, e], a, lax.rem(b + e, B), tp,
            )
            for e in range(1, B)
        ]

    def w_forward(i, d):
        wz[i, d].wait_recv()
        ref = weights[i][1].at[d_rows(a_from(d), b), :]
        wx[i, d] = [
            remote(ref, ref, wx_s.at[i, d, e], wx_r.at[i, d, e], a, lax.rem(b + e, B), tp)
            for e in range(1, B)
        ]

    heads = CH // HEAD_DIM
    query = jnp.concatenate(
        [
            turn(
                q_ref[:, i * HEAD_DIM : (i + 1) * HEAD_DIM],
                qg_ref[...], cos_ref[...], sin_ref[...],
            )
            for i in range(heads)
        ],
        axis=0,
    )
    factor2 = HEAD_DIM**-0.5 * math.log2(math.e)
    keys_at_once = min(B, 2) * R
    state = (
        jnp.full((heads * R, 1), -1e30, jnp.float32),
        jnp.zeros((heads * R, 1), jnp.float32),
        jnp.zeros((heads * R, HEAD_DIM), jnp.float32),
    )
    for d in range(A):
        for copy in kvx[d]:
            copy.wait_recv()
        if d + 1 < A:
            kvz[d + 1].wait_recv()
            kvx[d + 1] = kv_forward(d + 1)

        def attend(step, carried, d=d):
            running, total, summed = carried
            at = pl.ds(
                pl.multiple_of(a_from(d) * (B * R) + step * keys_at_once, R), keys_at_once
            )
            scores = lax.dot_general(
                query, kv[0, at, :], (((1,), (1,)), ((), ())),
                preferred_element_type=jnp.float32,
            )
            newest = jnp.maximum(running, jnp.max(scores, axis=-1, keepdims=True))
            scale = jnp.exp2((running - newest) * factor2)
            exps = jnp.exp2((scores - newest) * factor2)
            total = total * scale + jnp.sum(exps, axis=-1, keepdims=True)
            summed = summed * scale + jnp.dot(
                exps.astype(jnp.bfloat16), kv[1, at, :], preferred_element_type=jnp.float32
            )
            return newest, total, summed

        steps = (B * R) // keys_at_once
        if steps == 1:
            state = attend(0, state)
        else:
            state = lax.fori_loop(0, steps, attend, state)
    attended = (state[2] / state[1]).astype(jnp.bfloat16)
    for i in range(heads):
        for t in range(NT):
            begin = i * R + t * Q
            att[t, :, i * HEAD_DIM : (i + 1) * HEAD_DIM] = attended[begin : begin + Q, :]

    here = pl.ds(pl.multiple_of(tp * CH, 128), CH)
    att_copies = []
    for e in range(1, NT):
        t_ = lax.rem(tp + e, NT)
        att_copies.append(
            remote(att.at[t_], att_in.at[:, here], at_s.at[e], at_r.at[e], a, b, t_)
        )
    att_in[:, here] = att[tp]
    locals_[0].wait()
    for copy in att_copies:
        copy.wait_recv()

    tile = 512

    def out_tile(n, carried):
        cols = pl.ds(pl.multiple_of(n * tile, tile), tile)
        mixed[:, cols] = jnp.dot(
            att_in[...], wo[:, cols], preferred_element_type=jnp.float32
        )
        return carried

    lax.fori_loop(0, D // tile, out_tile, 0)
    first = layer_norm(
        RESIDUAL_SCALE * res_ref[...].astype(jnp.float32) + mixed[...], g1_ref[...], b1_ref[...]
    ).astype(jnp.bfloat16)
    own_rows = tok_rows(a, h, l)
    rows[own_rows, :] = first

    gz, gh, gl = {}, {}, {}
    for d in range(1, A):
        ref = rows.at[own_rows, :]
        gz[d] = remote(ref, ref, gz_s.at[d], gz_r.at[d], a_to(d), b, tp)

    def gl_forward(d, e):
        ref = rows.at[tok_rows(a_from(d), lax.rem(h + H - e, H), l), :]
        gl[d, e] = remote(ref, ref, gl_s.at[d, e], gl_r.at[d, e], a, b, h * L + (1 - l))

    def gh_forward(d):
        ref = rows.at[tok_rows(a_from(d), h, l), :]
        for e in range(1, H):
            gh[d, e] = remote(
                ref, ref, gh_s.at[d, e], gh_r.at[d, e], a, b, lax.rem(h + e, H) * L + l
            )
        gl_forward(d, 0)

    w_send(1)
    gh_forward(0)
    for d in range(1, A):
        w_forward(0, d)
    locals_[1].wait()

    block = NT * Q

    def up_block(g):
        for e in range(H):
            gl[g, e].wait_recv()
        at = pl.ds(pl.multiple_of(a_from(g) * block, block), block)
        up = jnp.dot(rows[at, :], wup[...], preferred_element_type=jnp.float32)
        hid[at, :] = jnp.square(jnp.maximum(up, 0.0)).astype(jnp.bfloat16)

    for d in range(1, A + 1):
        if d < A:
            gz[d].wait_recv()
            gh_forward(d)
        for e in range(1, H):
            gh[d - 1, e].wait_recv()
            gl_forward(d - 1, e)
    for d in range(A):
        for copy in wx[0, d]:
            copy.wait_recv()
    for d in range(A):
        up_block(d)
    locals_[2].wait()

    cols_of = B * DB
    lsend, hsend, zsend = {}, {}, {}

    def down_tile(d):
        for copy in wx[1, d]:
            copy.wait_recv()
        cols = pl.ds(pl.multiple_of(a_from(d) * cols_of, cols_of), cols_of)

        def one(o, carried):
            at = pl.ds(pl.multiple_of(o * block, block), block)
            piece = lax.dot_general(
                hid[at, :], wdn[cols, :], (((1,), (1,)), ((), ())),
                preferred_element_type=jnp.float32,
            ).astype(jnp.bfloat16)
            for h_ in range(H):
                for l_ in range(L):
                    begin = (h_ * L + l_) * Q
                    part[d, l_, h_, o] = piece[begin : begin + Q, :]
            return carried

        lax.fori_loop(0, A, one, 0)
        lsend[d] = remote(
            part.at[d, 1 - l], rl.at[d], rl_s.at[d], rl_r.at[d], a, b, h * L + (1 - l)
        )

    def core_sum(d):
        lsend[d].wait_recv()

        def one(o, carried):
            for h_ in range(H):
                s1[d, h_, o] = (
                    part[d, l, h_, o].astype(jnp.float32) + rl[d, h_, o].astype(jnp.float32)
                ).astype(jnp.bfloat16)
            return carried

        lax.fori_loop(0, A, one, 0)
        for e in range(1, H):
            h_ = lax.rem(h + e, H)
            hsend[d, e] = remote(
                s1.at[d, h_], rh.at[d, e], rh_s.at[d, e], rh_r.at[d, e], a, b, h_ * L + l
            )

    def tp_sum(d):
        for e in range(1, H):
            hsend[d, e].wait_recv()
        n = a_from(d)
        cols = pl.ds(pl.multiple_of(n * cols_of, 128), cols_of)
        for k in list(range(1, A)) + [0]:
            o = a_to(k)
            total = s1[d, h, o].astype(jnp.float32)
            for e in range(1, H):
                total = total + rh[d, e, o].astype(jnp.float32)
            if k == 0:
                mixed[:, cols] = total
                continue
            s2[d, k] = total.astype(jnp.bfloat16)
            zsend[d, k] = remote(
                s2.at[d, k], rz.at[k, :, cols], rz_s.at[d, k], rz_r.at[n, k], o, b, tp
            )

    for d in range(A):
        if d > 0:
            w_forward(1, d)
            core_sum(d - 1)
        down_tile(d)
        if d > 1:
            tp_sum(d - 2)
    core_sum(A - 1)
    for d in range(max(A - 2, 0), A):
        tp_sum(d)
    total = mixed[...]
    for k in range(1, A):
        for n in range(A):
            own = pl.ds(n * cols_of, cols_of)
            pltpu.make_async_remote_copy(
                src_ref=s2.at[n, k], dst_ref=rz.at[k, :, own], send_sem=rz_s.at[n, k],
                recv_sem=rz_r.at[n, k], device_id={"sp": a_to(k) * B + b, "tp": tp}, device_id_type=MESH,
            ).wait_recv()
        total = total + rz[k].astype(jnp.float32)
    out_ref[...] = layer_norm(
        RESIDUAL_SCALE * rows[own_rows, :].astype(jnp.float32) + total,
        g2_ref[...], b2_ref[...],
    ).astype(jnp.bfloat16)
    for copy in sends:
        copy.wait_send()


def per_device(
    sp_size, tp_size,
    queries, keys, values, residual, query_gain, key_gain, out_weight,
    first_gain, first_bias, up_weight, down_weight, second_gain, second_bias,
):
    A = math.gcd(sp_size, 4)
    B = sp_size // A
    L = 2
    H = tp_size // L
    R, CH = queries.shape
    Q, D = residual.shape
    DB, FFL = up_weight.shape
    W = FFL // A
    T = R * sp_size
    block = tp_size * Q
    positions = lax.axis_index("sp") * R + jnp.arange(R, dtype=jnp.int32)
    cosine, sine = grid_tables(positions)
    dma = pltpu.SemaphoreType.DMA
    bf, f32 = jnp.bfloat16, jnp.float32
    vmem = pl.BlockSpec(memory_space=pltpu.VMEM)
    hbm = pl.BlockSpec(memory_space=pl.ANY)
    scratch = [
        pltpu.VMEM((2, T, HEAD_DIM), bf),
        pltpu.VMEM((D, W), bf),
        pltpu.VMEM((D, W), bf),
        pltpu.VMEM(out_weight.shape, bf),
        pltpu.VMEM((tp_size, Q, CH), bf),
        pltpu.VMEM((Q, tp_size * CH), bf),
        pltpu.VMEM((Q, D), f32),
        pltpu.VMEM((A * block, D), bf),
        pltpu.VMEM((A * block, W), bf),
        pltpu.VMEM((A, L, H, A, Q, D // A), bf),
        pltpu.VMEM((A, H, A, Q, D // A), bf),
        pltpu.VMEM((A, H, A, Q, D // A), bf),
        pltpu.VMEM((A, H, A, Q, D // A), bf),
        pltpu.VMEM((A, A, Q, D // A), bf),
        pltpu.VMEM((A, Q, D), bf),
        dma((3,)),
        dma((A,)), dma((A,)), dma((A, B)), dma((A, B)),
        dma((2, A)), dma((2, A)), dma((2, A, B)), dma((2, A, B)),
        dma((tp_size,)), dma((tp_size,)),
        dma((A,)), dma((A,)), dma((A, H)), dma((A, H)), dma((A, H)), dma((A, H)),
        dma((A,)), dma((A,)), dma((A, H)), dma((A, H)), dma((A, A)), dma((A, A)),
    ]
    as_row = lambda x: x.reshape(1, -1)
    return pl.pallas_call(
        functools.partial(kernel, (A, B, H)),
        out_shape=jax.ShapeDtypeStruct((Q, D), bf),
        in_specs=[vmem] * 8 + [hbm] + [vmem] * 2 + [hbm] * 2 + [vmem] * 2,
        out_specs=vmem,
        scratch_shapes=scratch,
        compiler_params=pltpu.CompilerParams(
            collective_id=0, has_side_effects=True, vmem_limit_bytes=60000 * 1024
        ),
        name="layer",
    )(
        queries, keys, values, residual, cosine, sine, as_row(query_gain), as_row(key_gain),
        out_weight, as_row(first_gain), as_row(first_bias), up_weight, down_weight,
        as_row(second_gain), as_row(second_bias),
    )


def solution(mesh):
    both = P("sp", "tp")
    split_rows = P(("sp", "tp"), None)
    in_specs = (
        both, both, both, split_rows, P(), P(), P(), P(), P(), both, both, P(), P(),
    )
    return jax.shard_map(
        functools.partial(per_device, mesh.shape["sp"], mesh.shape["tp"]),
        mesh=mesh, in_specs=in_specs, out_specs=split_rows, check_vma=False,
    )
```

```python
import functools
import math

import jax
import jax.numpy as jnp
from jax import lax
from jax.experimental import pallas as pl
from jax.experimental.pallas import tpu as pltpu
from jax.sharding import PartitionSpec as P

HEAD_DIM = 128
GRID_W = 64
RESIDUAL_SCALE = 2.0**0.25
LAYER_EPS = 1e-05
HEAD_EPS = 1e-06
ROTARY_BASE = 10000.0
MESH = pl.DeviceIdType.MESH


def grid_tables(positions):
    quarter = HEAD_DIM // 4
    lane = jnp.arange(HEAD_DIM, dtype=jnp.int32)
    pair = lane // 2
    inverse = ROTARY_BASE ** (-(pair % quarter).astype(jnp.float32) / quarter)
    grid_row = (positions // GRID_W).astype(jnp.float32)
    grid_col = (positions % GRID_W).astype(jnp.float32)
    angles = jnp.where(pair < quarter, grid_row[:, None], grid_col[:, None]) * inverse
    sign = jnp.where(lane % 2 == 0, -1.0, 1.0)
    return jnp.cos(angles), jnp.sin(angles) * sign


def turn(block, gain, cosine, sine):
    x = block.astype(jnp.float32)
    x = x * lax.rsqrt(jnp.mean(x * x, axis=-1, keepdims=True) + HEAD_EPS) * gain
    lane = lax.broadcasted_iota(jnp.int32, x.shape, 1)
    swapped = jnp.where(
        lane % 2 == 0, pltpu.roll(x, HEAD_DIM - 1, 1), pltpu.roll(x, 1, 1)
    )
    return (x * cosine + swapped * sine).astype(jnp.bfloat16)


def layer_norm(summed, gain, bias):
    centred = summed - jnp.mean(summed, axis=-1, keepdims=True)
    variance = jnp.mean(centred * centred, axis=-1, keepdims=True)
    return centred * lax.rsqrt(variance + LAYER_EPS) * gain + bias


def kernel(
    dims,
    q_ref, k_ref, v_ref, res_ref, cos_ref, sin_ref, qg_ref, kg_ref, wo_hbm,
    g1_ref, b1_ref, up_hbm, down_hbm, g2_ref, b2_ref,
    out_ref,
    kv, wup, wdn, wo, att, att_in, mixed, rows, hid, part, rl, s1, rh, s2, rz,
    local_sem, kvz_s, kvz_r, kvx_s, kvx_r, wz_s, wz_r, wx_s, wx_r,
    at_s, at_r, gz_s, gz_r, gh_s, gh_r, gl_s, gl_r,
    rl_s, rl_r, rh_s, rh_r, rz_s, rz_r,
):
    A, B, H = dims
    L = 2
    NT = H * L
    R = q_ref.shape[0]
    CH = q_ref.shape[1]
    Q = R // NT
    D = wup.shape[0]
    DB = up_hbm.shape[0]
    W = wup.shape[1]
    sp = lax.axis_index("sp")
    tp = lax.axis_index("tp")
    a, b = lax.div(sp, B), lax.rem(sp, B)
    h, l = lax.div(tp, L), lax.rem(tp, L)
    sends = []

    def a_to(d):
        return lax.rem(a + d, A)

    def a_from(d):
        return lax.rem(a + A - d, A)

    def remote(src, dst, ssem, rsem, a_, b_, t_):
        copy = pltpu.make_async_remote_copy(
            src_ref=src, dst_ref=dst, send_sem=ssem, recv_sem=rsem,
            device_id={"sp": a_ * B + b_, "tp": t_}, device_id_type=MESH,
        )
        copy.start()
        sends.append(copy)
        return copy

    def ff_cols(a_):
        return pl.ds(pl.multiple_of(a_ * W, 128), W)

    def d_rows(a_, b_):
        return pl.ds(pl.multiple_of((a_ * B + b_) * DB, DB), DB)

    def kv_rows(a_, b_):
        return pl.ds(pl.multiple_of((a_ * B + b_) * R, R), R)

    def tok_rows(a_, h_, l_):
        return pl.ds(pl.multiple_of(((a_ * H + h_) * L + l_) * Q, Q), Q)

    weights = ((up_hbm, wup), (down_hbm, wdn))
    locals_ = [pltpu.make_async_copy(wo_hbm, wo, local_sem.at[0])]
    for i, (src, dst) in enumerate(weights):
        locals_.append(
            pltpu.make_async_copy(
                src.at[:, ff_cols(a)], dst.at[d_rows(a, b), :], local_sem.at[1 + i]
            )
        )
    for copy in locals_:
        copy.start()

    barrier = pltpu.get_barrier_semaphore()
    peers = [(a_to(d), b, tp) for d in range(1, A)]
    peers += [(a, lax.rem(b + e, B), tp) for e in range(1, B)]
    peers += [(a, b, lax.rem(tp + e, NT)) for e in range(1, NT)]
    for a_, b_, t_ in peers:
        pl.semaphore_signal(
            barrier, inc=1, device_id={"sp": a_ * B + b_, "tp": t_}, device_id_type=MESH
        )

    mine = kv_rows(a, b)
    kv[0, mine, :] = turn(k_ref[...], kg_ref[...], cos_ref[...], sin_ref[...])
    kv[1, mine, :] = v_ref[...]
    pl.semaphore_wait(barrier, len(peers))

    kvz = {}
    for d in range(1, A):
        ref = kv.at[:, kv_rows(a, b), :]
        kvz[d] = remote(ref, ref, kvz_s.at[d], kvz_r.at[d], a_to(d), b, tp)

    def kv_forward(d):
        ref = kv.at[:, kv_rows(a_from(d), b), :]
        return [
            remote(ref, ref, kvx_s.at[d, e], kvx_r.at[d, e], a, lax.rem(b + e, B), tp)
            for e in range(1, B)
        ]

    kvx = {0: kv_forward(0)}
    wz, wx = {}, {}
    def w_send(i):
        src, dst = weights[i]
        for d in range(1, A):
            wz[i, d] = remote(
                src.at[:, ff_cols(a_to(d))], dst.at[d_rows(a, b), :],
                wz_s.at[i, d], wz_r.at[i, d], a_to(d), b, tp,
            )

    def w_own():
        for i, (src, dst) in enumerate(weights):
            wx[i, 0] = [
                remote(
                    src.at[:, ff_cols(a)], dst.at[d_rows(a, b), :],
                    wx_s.at[i, 0, e], wx_r.at[i, 0, e], a, lax.rem(b + e, B), tp,
                )
                for e in range(1, B)
            ]

    def w_forward(i, d):
        wz[i, d].wait_recv()
        ref = weights[i][1].at[d_rows(a_from(d), b), :]
        wx[i, d] = [
            remote(ref, ref, wx_s.at[i, d, e], wx_r.at[i, d, e], a, lax.rem(b + e, B), tp)
            for e in range(1, B)
        ]

    heads = CH // HEAD_DIM
    query = jnp.concatenate(
        [
            turn(
                q_ref[:, i * HEAD_DIM : (i + 1) * HEAD_DIM],
                qg_ref[...], cos_ref[...], sin_ref[...],
            )
            for i in range(heads)
        ],
        axis=0,
    )
    factor2 = HEAD_DIM**-0.5 * math.log2(math.e)
    keys_at_once = min(B, 2) * R
    state = (
        jnp.full((heads * R, 1), -1e30, jnp.float32),
        jnp.zeros((heads * R, 1), jnp.float32),
        jnp.zeros((heads * R, HEAD_DIM), jnp.float32),
    )
    for d in range(A):
        for copy in kvx[d]:
            copy.wait_recv()
        if d + 1 < A:
            kvz[d + 1].wait_recv()
            kvx[d + 1] = kv_forward(d + 1)
        if d == 0:
            w_send(0)
        if d == max(A - 2, 0):
            w_own()

        def attend(step, carried, d=d):
            running, total, summed = carried
            at = pl.ds(
                pl.multiple_of(a_from(d) * (B * R) + step * keys_at_once, R), keys_at_once
            )
            scores = lax.dot_general(
                query, kv[0, at, :], (((1,), (1,)), ((), ())),
                preferred_element_type=jnp.float32,
            )
            newest = jnp.maximum(running, jnp.max(scores, axis=-1, keepdims=True))
            scale = jnp.exp2((running - newest) * factor2)
            exps = jnp.exp2((scores - newest) * factor2)
            total = total * scale + jnp.sum(exps, axis=-1, keepdims=True)
            summed = summed * scale + jnp.dot(
                exps.astype(jnp.bfloat16), kv[1, at, :], preferred_element_type=jnp.float32
            )
            return newest, total, summed

        steps = (B * R) // keys_at_once
        if steps == 1:
            state = attend(0, state)
        else:
            state = lax.fori_loop(0, steps, attend, state)
    attended = (state[2] / state[1]).astype(jnp.bfloat16)
    for i in range(heads):
        for t in range(NT):
            begin = i * R + t * Q
            att[t, :, i * HEAD_DIM : (i + 1) * HEAD_DIM] = attended[begin : begin + Q, :]

    here = pl.ds(pl.multiple_of(tp * CH, 128), CH)
    att_copies = []
    for e in range(1, NT):
        t_ = lax.rem(tp + e, NT)
        att_copies.append(
            remote(att.at[t_], att_in.at[:, here], at_s.at[e], at_r.at[e], a, b, t_)
        )
    att_in[:, here] = att[tp]
    locals_[0].wait()
    for copy in att_copies:
        copy.wait_recv()

    tile = 512

    def out_tile(n, carried):
        cols = pl.ds(pl.multiple_of(n * tile, tile), tile)
        mixed[:, cols] = jnp.dot(
            att_in[...], wo[:, cols], preferred_element_type=jnp.float32
        )
        return carried

    lax.fori_loop(0, D // tile, out_tile, 0)
    first = layer_norm(
        RESIDUAL_SCALE * res_ref[...].astype(jnp.float32) + mixed[...], g1_ref[...], b1_ref[...]
    ).astype(jnp.bfloat16)
    own_rows = tok_rows(a, h, l)
    rows[own_rows, :] = first

    gz, gh, gl = {}, {}, {}
    for d in range(1, A):
        ref = rows.at[own_rows, :]
        gz[d] = remote(ref, ref, gz_s.at[d], gz_r.at[d], a_to(d), b, tp)

    def gl_forward(d, e):
        ref = rows.at[tok_rows(a_from(d), lax.rem(h + H - e, H), l), :]
        gl[d, e] = remote(ref, ref, gl_s.at[d, e], gl_r.at[d, e], a, b, h * L + (1 - l))

    def gh_forward(d):
        ref = rows.at[tok_rows(a_from(d), h, l), :]
        for e in range(1, H):
            gh[d, e] = remote(
                ref, ref, gh_s.at[d, e], gh_r.at[d, e], a, b, lax.rem(h + e, H) * L + l
            )
        gl_forward(d, 0)

    w_send(1)
    gh_forward(0)
    for d in range(1, A):
        w_forward(0, d)
    locals_[1].wait()

    block = NT * Q

    def up_block(g):
        for e in range(H):
            gl[g, e].wait_recv()
        at = pl.ds(pl.multiple_of(a_from(g) * block, block), block)
        up = jnp.dot(rows[at, :], wup[...], preferred_element_type=jnp.float32)
        hid[at, :] = jnp.square(jnp.maximum(up, 0.0)).astype(jnp.bfloat16)

    for d in range(1, A + 1):
        if d < A:
            gz[d].wait_recv()
            gh_forward(d)
        for e in range(1, H):
            gh[d - 1, e].wait_recv()
            gl_forward(d - 1, e)
    for d in range(A):
        for copy in wx[0, d]:
            copy.wait_recv()
    for d in range(A):
        up_block(d)
    locals_[2].wait()

    S = part.shape[0] // A
    cols_of = D // (A * S)
    lsend, hsend, zsend = {}, {}, {}

    def first_col(d, e):
        if S == 1:
            return a_from(d) * cols_of
        return (a_from(d) * B + lax.rem(b + B - e, B)) * cols_of

    def down_tile(d):
        outer, inner = divmod(d, S)
        if S == 1:
            for copy in wx[1, outer]:
                copy.wait_recv()
        elif inner > 0:
            wx[1, outer][inner - 1].wait_recv()
        cols = pl.ds(pl.multiple_of(first_col(outer, inner), cols_of), cols_of)

        def one(o, carried):
            at = pl.ds(pl.multiple_of(o * block, block), block)
            piece = lax.dot_general(
                hid[at, :], wdn[cols, :], (((1,), (1,)), ((), ())),
                preferred_element_type=jnp.float32,
            ).astype(jnp.bfloat16)
            for h_ in range(H):
                for l_ in range(L):
                    begin = (h_ * L + l_) * Q
                    part[d, l_, h_, o] = piece[begin : begin + Q, :]
            return carried

        lax.fori_loop(0, A, one, 0)
        lsend[d] = remote(
            part.at[d, 1 - l], rl.at[d], rl_s.at[d], rl_r.at[d], a, b, h * L + (1 - l)
        )

    def core_sum(d):
        lsend[d].wait_recv()

        def one(o, carried):
            for h_ in range(H):
                s1[d, h_, o] = (
                    part[d, l, h_, o].astype(jnp.float32) + rl[d, h_, o].astype(jnp.float32)
                ).astype(jnp.bfloat16)
            return carried

        lax.fori_loop(0, A, one, 0)
        for e in range(1, H):
            h_ = lax.rem(h + e, H)
            hsend[d, e] = remote(
                s1.at[d, h_], rh.at[d, e], rh_s.at[d, e], rh_r.at[d, e], a, b, h_ * L + l
            )

    def tp_sum(d):
        for e in range(1, H):
            hsend[d, e].wait_recv()
        begin = first_col(d // S, d % S)
        n = lax.div(begin, cols_of)
        cols = pl.ds(pl.multiple_of(begin, 128), cols_of)
        for k in list(range(1, A)) + [0]:
            o = a_to(k)
            total = s1[d, h, o].astype(jnp.float32)
            for e in range(1, H):
                total = total + rh[d, e, o].astype(jnp.float32)
            if k == 0:
                mixed[:, cols] = total
                continue
            s2[d, k] = total.astype(jnp.bfloat16)
            zsend[d, k] = remote(
                s2.at[d, k], rz.at[k, :, cols], rz_s.at[d, k], rz_r.at[k, n], o, b, tp
            )

    tiles = A * S
    for d in range(tiles):
        if d > 0 and d % S == 0:
            w_forward(1, d // S)
        down_tile(d)
        if d > 0:
            core_sum(d - 1)
        if d > 1:
            tp_sum(d - 2)
    core_sum(tiles - 1)
    for d in range(max(tiles - 2, 0), tiles):
        tp_sum(d)
    total = mixed[...]
    for k in range(1, A):
        for n in range(tiles):
            own = pl.ds(n * cols_of, cols_of)
            pltpu.make_async_remote_copy(
                src_ref=s2.at[n, k], dst_ref=rz.at[k, :, own], send_sem=rz_s.at[n, k],
                recv_sem=rz_r.at[k, n], device_id={"sp": a_to(k) * B + b, "tp": tp}, device_id_type=MESH,
            ).wait_recv()
        total = total + rz[k].astype(jnp.float32)
    out_ref[...] = layer_norm(
        RESIDUAL_SCALE * rows[own_rows, :].astype(jnp.float32) + total,
        g2_ref[...], b2_ref[...],
    ).astype(jnp.bfloat16)
    for copy in sends:
        copy.wait_send()


def per_device(
    sp_size, tp_size,
    queries, keys, values, residual, query_gain, key_gain, out_weight,
    first_gain, first_bias, up_weight, down_weight, second_gain, second_bias,
):
    A = math.gcd(sp_size, 4)
    B = sp_size // A
    L = 2
    H = tp_size // L
    R, CH = queries.shape
    Q, D = residual.shape
    DB, FFL = up_weight.shape
    W = FFL // A
    T = R * sp_size
    block = tp_size * Q
    S = B if DB % 128 == 0 else 1
    tiles, C = A * S, D // (A * S)
    positions = lax.axis_index("sp") * R + jnp.arange(R, dtype=jnp.int32)
    cosine, sine = grid_tables(positions)
    dma = pltpu.SemaphoreType.DMA
    bf, f32 = jnp.bfloat16, jnp.float32
    vmem = pl.BlockSpec(memory_space=pltpu.VMEM)
    hbm = pl.BlockSpec(memory_space=pl.ANY)
    scratch = [
        pltpu.VMEM((2, T, HEAD_DIM), bf),
        pltpu.VMEM((D, W), bf),
        pltpu.VMEM((D, W), bf),
        pltpu.VMEM(out_weight.shape, bf),
        pltpu.VMEM((tp_size, Q, CH), bf),
        pltpu.VMEM((Q, tp_size * CH), bf),
        pltpu.VMEM((Q, D), f32),
        pltpu.VMEM((A * block, D), bf),
        pltpu.VMEM((A * block, W), bf),
        pltpu.VMEM((tiles, L, H, A, Q, C), bf),
        pltpu.VMEM((tiles, H, A, Q, C), bf),
        pltpu.VMEM((tiles, H, A, Q, C), bf),
        pltpu.VMEM((tiles, H, A, Q, C), bf),
        pltpu.VMEM((tiles, A, Q, C), bf),
        pltpu.VMEM((A, Q, D), bf),
        dma((3,)),
        dma((A,)), dma((A,)), dma((A, B)), dma((A, B)),
        dma((2, A)), dma((2, A)), dma((2, A, B)), dma((2, A, B)),
        dma((tp_size,)), dma((tp_size,)),
        dma((A,)), dma((A,)), dma((A, H)), dma((A, H)), dma((A, H)), dma((A, H)),
        dma((tiles,)), dma((tiles,)), dma((tiles, H)), dma((tiles, H)),
        dma((tiles, A)), dma((A, tiles)),
    ]
    as_row = lambda x: x.reshape(1, -1)
    return pl.pallas_call(
        functools.partial(kernel, (A, B, H)),
        out_shape=jax.ShapeDtypeStruct((Q, D), bf),
        in_specs=[vmem] * 8 + [hbm] + [vmem] * 2 + [hbm] * 2 + [vmem] * 2,
        out_specs=vmem,
        scratch_shapes=scratch,
        compiler_params=pltpu.CompilerParams(
            collective_id=0, has_side_effects=True, vmem_limit_bytes=60000 * 1024
        ),
        name="layer",
    )(
        queries, keys, values, residual, cosine, sine, as_row(query_gain), as_row(key_gain),
        out_weight, as_row(first_gain), as_row(first_bias), up_weight, down_weight,
        as_row(second_gain), as_row(second_bias),
    )


def solution(mesh):
    both = P("sp", "tp")
    split_rows = P(("sp", "tp"), None)
    in_specs = (
        both, both, both, split_rows, P(), P(), P(), P(), P(), both, both, P(), P(),
    )
    return jax.shard_map(
        functools.partial(per_device, mesh.shape["sp"], mesh.shape["tp"]),
        mesh=mesh, in_specs=in_specs, out_specs=split_rows, check_vma=False,
    )
```
